32 devices in a mesh: fs: 8 (over z, y), tp: 4 (over x, core).
Axes of the slice: x: 2, y: 2, z: 4, core: 2. Of those that a mesh axis runs over, the one named last changes fastest.
Arguments:
- tokens: bfloat16 [8192, 2048], P('fs'), may hold values from -6 to 6
- norm_gain: float32 [2048], replicated, may hold values from 0.1 to 1.9
- gate_weight: bfloat16 [2048, 4096], P('fs', 'tp'), may hold values from -0.125 to 0.125
- up_weight: bfloat16 [2048, 4096], P('fs', 'tp'), may hold values from -0.125 to 0.125
- down_weight: bfloat16 [4096, 2048], P('tp', 'fs'), may hold values from -2 to 2
- out_gain: float32 [2048], P('tp'), may hold values from 0.1 to 1.9
Outputs:
- result: bfloat16 [8192, 2048], P('fs', 'tp')
The draws below stay inside these ranges and needn't reach their ends.
All inputs are finite; a program needn't handle non-finite values.
Results may differ from the reference program's by a relative error of at most 0.014.
Values may be sent and summed in bfloat16 or wider, within the bound.
A program may use at most 64 MiB of HBM per device.

```python
import jax
import jax.numpy as jnp
from jax import lax

D = 2048
FF = 4096
TOK_DEV = 1024
TOKENS = 8192
N_FS = 8
N_TP = 4


def draw_down_weight(key, part):
    first_key, second_key = jax.random.split(jax.random.fold_in(key, 17))
    group_scales = jnp.exp(jax.random.uniform(second_key, (16,), jnp.float32, -0.9, 0.9))
    column_scale = jnp.repeat(group_scales, D // 16)
    base = jnp.clip(jax.random.normal(first_key, (FF, D), jnp.float32), -4.0, 4.0)
    values = jnp.clip(base * FF ** (-0.5) * column_scale[None, :], -2.0, 2.0)
    return values.astype(jnp.bfloat16)


def shard_levels(key, shape, cuts, low, largest):
    def one(position, parts):
        steps = jax.random.uniform(jax.random.fold_in(jax.random.fold_in(key, 6), position), (parts,), jnp.float32, low / len(cuts), largest / len(cuts))
        return jnp.repeat(jnp.exp(steps), shape[position] // parts).reshape((-1,) + (1,) * (len(shape) - position - 1))

    gain = one(*cuts[0])
    for cut in cuts[1:]:
        gain = gain * one(*cut)
    return gain


def normal_values(own_key, shape, spread, reach, cuts=(), dtype=jnp.bfloat16):
    drawn = spread * jax.random.normal(own_key, shape, jnp.float32)
    if cuts:
        drawn = drawn * shard_levels(own_key, shape, cuts, -0.22, 0.18)
    return jnp.clip(drawn, -reach, reach).astype(dtype)


def setup_inputs(seed: int = 0) -> dict:
    key_list = jax.random.split(jax.random.key(seed), 7)
    return {
        "tokens": normal_values(key_list[0], (TOKENS, D), 1.0, 6.0, ((0, 8),)),
        "norm_gain": jnp.clip(1.0 + 0.18 * jax.random.normal(key_list[1], (D,), jnp.float32), 0.1, 1.9),
        "gate_weight": normal_values(key_list[2], (D, FF), D ** -0.5, 0.125, ((0, 8), (1, 4))),
        "up_weight": normal_values(key_list[3], (D, FF), D ** -0.5, 0.125, ((0, 8), (1, 4))),
        "down_weight": draw_down_weight(jax.random.fold_in(key_list[6], 71), 0),
        "out_gain": jnp.clip(1.0 + 0.18 * jax.random.normal(key_list[5], (D,), jnp.float32), 0.1, 1.9),
    }


EPSILON = 1e-06

def reference(tokens, norm_gain, gate_weight, up_weight, down_weight, out_gain):
    width = FF // N_TP
    down_blocks = down_weight.reshape(N_TP, width, D)

    def one_block(rows):
        values = rows.astype(jnp.float32)
        normed = (values * lax.rsqrt(lax.optimization_barrier(jnp.mean(values * values, axis=1, keepdims=True)) + EPSILON) * norm_gain.astype(jnp.float32)).astype(jnp.bfloat16)
        gate_proj = jnp.dot(normed, gate_weight, preferred_element_type=jnp.float32)
        up_proj = jnp.dot(normed, up_weight, preferred_element_type=jnp.float32)
        hidden = (jax.nn.silu(gate_proj) * up_proj).astype(jnp.bfloat16)
        branch = jnp.zeros((rows.shape[0], D), jnp.float32)
        for index in range(N_TP):
            piece = jnp.dot(hidden[:, index * width:(index + 1) * width], down_blocks[index], preferred_element_type=jnp.float32).astype(jnp.bfloat16)
            branch = branch + lax.optimization_barrier(piece).astype(jnp.float32)
        mean_square = lax.optimization_barrier(jnp.mean(branch * branch, axis=1, keepdims=True))
        return (branch * lax.rsqrt(mean_square + EPSILON) * out_gain.astype(jnp.float32)).astype(jnp.bfloat16)
    blocks = tokens.reshape(N_FS, TOK_DEV, D)
    return lax.map(one_block, blocks).reshape(TOKENS, D)
```

```python
import functools

import jax
import jax.numpy as jnp
from jax import lax
from jax.experimental import pallas as pl
from jax.experimental.pallas import tpu as pltpu
from jax.sharding import PartitionSpec as P

EPSILON = 1e-06
MESH = pl.DeviceIdType.MESH
PIECES = 4
COLUMN_TILE = 256


def ring_layout(n, n_tp):
    ny = max(n_tp // 2, 1)
    if n % ny or (n // ny) % 2:
        ny = 1
    nz, rest = n // ny, max(ny - 1, 1)

    def position(fs):
        z, y = fs // ny, fs % ny
        k = nz - 1 - z
        odd = k % 2
        back = nz + k * rest + (1 - odd) * (y - 1) + odd * (ny - 1 - y)
        return jnp.where(y == 0, z, back)

    def index(pos):
        q = jnp.maximum(pos - nz, 0)
        k, r = q // rest, q % rest
        odd = k % 2
        back = (nz - 1 - k) * ny + (1 - odd) * (1 + r) + odd * (ny - 1 - r)
        return jnp.where(pos < nz, pos * ny, back)

    return position, index


def kernel(
    n, n_tp, tokens_hbm, norm_gain, gate_hbm, up_hbm, down_hbm, out_gain, out_ref,
    tok, normed, gate, up, down, gate_acc, up_acc, hidden, parts, sib, far, own, sq, sq_all,
    local_sem, ring_send, ring_recv, sib_send, sib_recv, far_send, far_recv, sq_send, sq_recv,
):
    half = n // 2
    nx, nb = n_tp // 2, n // n_tp
    n_tok, d_model = tok.shape
    rows_in = gate.shape[1]
    n_hid, width = down.shape[1], down.shape[2]
    piece = n_tok // PIECES
    position, index = ring_layout(n, n_tp)
    fs, tp = lax.axis_index("fs"), lax.axis_index("tp")
    x, core = tp // 2, tp % 2
    me = position(fs)
    block_of = {}
    for h in range(half + 1):
        block_of[0, h] = index((me + n - h) % n)
        block_of[1, h] = index((me + h) % n)
    target = (block_of[1, 1], block_of[0, 1])
    sibling = x * 2 + 1 - core

    barrier = pltpu.get_barrier_semaphore()
    for fs_id in target:
        pl.semaphore_signal(barrier, inc=1, device_id={"fs": fs_id}, device_id_type=MESH)
    for d in range(1, n_tp):
        pl.semaphore_signal(
            barrier, inc=1, device_id={"tp": (tp + d) % n_tp}, device_id_type=MESH
        )
    loads = [
        pltpu.make_async_copy(tokens_hbm, tok, local_sem.at[0]),
        pltpu.make_async_copy(gate_hbm, gate.at[fs], local_sem.at[1]),
        pltpu.make_async_copy(up_hbm, up.at[fs], local_sem.at[2]),
        pltpu.make_async_copy(down_hbm, down.at[fs], local_sem.at[3]),
    ]
    for load in loads:
        load.start()
    pl.semaphore_wait(barrier, 2 + n_tp - 1)

    def view(c, b, h, way):
        if c < 2:
            ref = (gate, up)[c]
            if h == half:
                return ref.at[b, pl.ds(way * (rows_in // 2), rows_in // 2)]
            return ref.at[b]
        return down.at[b, pl.ds((c - 2) * (n_hid // 2), n_hid // 2)]

    def ring_copy(c, way, h, b, first=False):
        dst = view(c, b, h, way)
        src = (gate_hbm, up_hbm)[c] if first and c < 2 else dst
        return pltpu.make_async_remote_copy(
            src_ref=src,
            dst_ref=dst,
            send_sem=ring_send.at[way, h - 1, c],
            recv_sem=ring_recv.at[way, h - 1, c],
            device_id={"fs": target[way]},
            device_id_type=MESH,
        )

    sends = []

    def send(c, way, h):
        copy = ring_copy(c, way, h, block_of[way, h - 1], h == 1)
        copy.start()
        sends.append(copy)

    def arrive(c, way, h):
        ring_copy(c, way, h, block_of[way, h]).wait_recv()

    for c in (0, 1):
        for way in (0, 1):
            send(c, way, 1)

    loads[0].wait()
    tile = min(128, n_tok)

    @pl.loop(0, n_tok // tile)
    def _(i):
        rows = pl.ds(pl.multiple_of(i * tile, tile), tile)
        v = tok[rows, :].astype(jnp.float32)
        r = lax.rsqrt(jnp.mean(v * v, axis=1, keepdims=True) + EPSILON)
        out = (v * r * norm_gain[...]).astype(jnp.bfloat16)
        for j in range(n):
            normed[j, rows, :] = out[:, j * rows_in:(j + 1) * rows_in]

    def accumulate(b, mode):
        n_col = gate.shape[2]
        step = min(COLUMN_TILE, n_col)

        @pl.loop(0, n_col // step)
        def _(i):
            cols = pl.ds(pl.multiple_of(i * step, step), step)
            a = normed[b]
            g = jnp.dot(a, gate[b, :, cols], preferred_element_type=jnp.float32)
            u = jnp.dot(a, up[b, :, cols], preferred_element_type=jnp.float32)
            if mode != "first":
                g = g + gate_acc[:, cols]
                u = u + up_acc[:, cols]
            if mode == "last":
                hidden[:, cols] = (g * (1.0 / (1.0 + jnp.exp(-g))) * u).astype(jnp.bfloat16)
            else:
                gate_acc[:, cols] = g
                up_acc[:, cols] = u

    loads[1].wait()
    loads[2].wait()
    accumulate(fs, "first")
    loads[3].wait()

    for h in range(1, half + 1):
        for c in (0, 1):
            for way in (0, 1):
                arrive(c, way, h)
                if h < half:
                    send(c, way, h + 1)
        if h == half - 1:
            for c in (2, 3):
                for way in (0, 1):
                    send(c, way, 1)
        if h < half:
            accumulate(block_of[0, h], "mid")
            accumulate(block_of[1, h], "mid")
        else:
            accumulate(block_of[0, h], "last")

    def owner(b):
        t = b // nb
        return t // 2, t % 2, b % nb

    def piece_rows(q):
        return pl.ds(pl.multiple_of(q * piece, piece), piece)

    def sib_copy(b, slot, q):
        return pltpu.make_async_remote_copy(
            src_ref=parts.at[b, piece_rows(q)],
            dst_ref=sib.at[slot, piece_rows(q)],
            send_sem=sib_send.at[slot, q],
            recv_sem=sib_recv.at[slot, q],
            device_id={"tp": sibling},
            device_id_type=MESH,
        )

    def far_copy(b, x_to, x_from, k, q):
        return pltpu.make_async_remote_copy(
            src_ref=parts.at[b, piece_rows(q)],
            dst_ref=far.at[x_from, k, piece_rows(q)],
            send_sem=far_send.at[x_to * nb + k, q],
            recv_sem=far_recv.at[x_from, k, q],
            device_id={"tp": x_to * 2 + core},
            device_id_type=MESH,
        )

    def multiply(b):
        x_to, core_to, k = owner(b)

        @pl.loop(0, PIECES)
        def _(q):
            rows = piece_rows(q)
            parts[b, rows, :] = jnp.dot(
                hidden[rows, :], down[b], preferred_element_type=jnp.float32
            ).astype(jnp.bfloat16)

            @pl.when(core_to != core)
            def _():
                sib_copy(b, x_to * nb + k, q).start()

    def reduce(b):
        x_to, core_to, k = owner(b)

        @pl.when((core_to == core) & (x_to != x))
        def _():
            @pl.loop(0, PIECES)
            def _(q):
                rows = piece_rows(q)
                slot = x_to * nb + k
                sib_copy(b, slot, q).wait_recv()
                parts[b, rows, :] = (
                    parts[b, rows, :].astype(jnp.float32) + sib[slot, rows, :].astype(jnp.float32)
                ).astype(jnp.bfloat16)
                far_copy(b, x_to, x, k, q).start()

    multiply(fs)
    pending = [fs]
    for h in range(1, half + 1):
        for c in (2, 3):
            for way in (0, 1):
                if h < half or way == c - 2:
                    arrive(c, way, h)
                if h < half - 1 or (h == half - 1 and way == c - 2):
                    send(c, way, h + 1)
            if c == 2:
                for b in pending:
                    reduce(b)
                pending = []
        for way in (0, 1) if h < half else (0,):
            multiply(block_of[way, h])
            pending.append(block_of[way, h])
    for b in pending:
        reduce(b)

    @pl.loop(0, PIECES)
    def _(q):
        rows = piece_rows(q)
        squares = jnp.zeros((piece, 1), jnp.float32)
        for k in range(nb):
            b, slot = tp * nb + k, x * nb + k
            v = parts[b, rows, :].astype(jnp.float32)
            sib_copy(b, slot, q).wait_recv()
            v = v + sib[slot, rows, :].astype(jnp.float32)
            for d in range(1, nx):
                x_from = (x + d) % nx
                far_copy(b, x, x_from, k, q).wait_recv()
                v = v + far[x_from, k, rows, :].astype(jnp.float32)
            own[k, rows, :] = v
            squares = squares + jnp.sum(v * v, axis=1, keepdims=True)
        sq[q] = jnp.transpose(jnp.broadcast_to(squares, (piece, 128)))[0:8, :]

    def sq_copy(to, slot):
        return pltpu.make_async_remote_copy(
            src_ref=sq,
            dst_ref=sq_all.at[slot],
            send_sem=sq_send.at[to],
            recv_sem=sq_recv.at[slot],
            device_id={"tp": to},
            device_id_type=MESH,
        )

    others = [(tp + d) % n_tp for d in range(1, n_tp)]
    for t in others:
        sq_copy(t, tp).start()
    for t in others:
        sq_copy(t, t).wait_recv()

    @pl.loop(0, PIECES)
    def _(q):
        rows = piece_rows(q)
        total = sq[q]
        for t in others:
            total = total + sq_all[t, q]
        r = lax.rsqrt(total / d_model + EPSILON)
        r = jnp.transpose(jnp.broadcast_to(r[0:1, :], (128, piece)))[:, 0:1]
        for k in range(nb):
            cols = slice(k * width, (k + 1) * width)
            out_ref[rows, cols] = (own[k, rows, :] * r * out_gain[:, cols]).astype(jnp.bfloat16)

    for t in others:
        sq_copy(t, tp).wait_send()
    for copy in sends:
        copy.wait_send()

    @pl.loop(0, PIECES)
    def _(q):
        for slot in range(nx * nb):
            sib_copy(slot, slot, q).wait_send()
        for d in range(1, nx):
            for k in range(nb):
                far_copy(k, (x + d) % nx, x, k, q).wait_send()


def body(n, n_tp, tokens, norm_gain, gate_weight, up_weight, down_weight, out_gain):
    n_tok, d_model = tokens.shape
    rows_in, n_hid = gate_weight.shape
    width = down_weight.shape[1]
    half, nx, nb = n // 2, n_tp // 2, n // n_tp
    piece = n_tok // PIECES
    bf16, f32 = jnp.bfloat16, jnp.float32
    dma = pltpu.SemaphoreType.DMA
    hbm = pl.BlockSpec(memory_space=pl.ANY)
    vmem = pl.BlockSpec(memory_space=pltpu.VMEM)
    return pl.pallas_call(
        functools.partial(kernel, n, n_tp),
        out_shape=jax.ShapeDtypeStruct((n_tok, out_gain.shape[0]), bf16),
        in_specs=[hbm, vmem, hbm, hbm, hbm, vmem],
        out_specs=vmem,
        scratch_shapes=[
            pltpu.VMEM((n_tok, d_model), bf16),
            pltpu.VMEM((n, n_tok, rows_in), bf16),
            pltpu.VMEM((n, rows_in, n_hid), bf16),
            pltpu.VMEM((n, rows_in, n_hid), bf16),
            pltpu.VMEM((n, n_hid, width), bf16),
            pltpu.VMEM((n_tok, n_hid), f32),
            pltpu.VMEM((n_tok, n_hid), f32),
            pltpu.VMEM((n_tok, n_hid), bf16),
            pltpu.VMEM((n, n_tok, width), bf16),
            pltpu.VMEM((nx * nb, n_tok, width), bf16),
            pltpu.VMEM((nx, nb, n_tok, width), bf16),
            pltpu.VMEM((nb, n_tok, width), f32),
            pltpu.VMEM((PIECES, 8, piece), f32),
            pltpu.VMEM((n_tp, PIECES, 8, piece), f32),
            dma((4,)),
            dma((2, half, 4)),
            dma((2, half, 4)),
            dma((nx * nb, PIECES)),
            dma((nx * nb, PIECES)),
            dma((nx * nb, PIECES)),
            dma((nx, nb, PIECES)),
            dma((n_tp,)),
            dma((n_tp,)),
        ],
        compiler_params=pltpu.CompilerParams(
            collective_id=0, has_side_effects=True, vmem_limit_bytes=62 * 1024 * 1024
        ),
        name="ffn_ring",
    )(tokens, norm_gain[None, :], gate_weight, up_weight, down_weight, out_gain[None, :])


def solution(mesh):
    return jax.shard_map(
        functools.partial(body, mesh.shape["fs"], mesh.shape["tp"]),
        mesh=mesh,
        in_specs=(P("fs", None), P(), P("fs", "tp"), P("fs", "tp"), P("tp", "fs"), P("tp")),
        out_specs=P("fs", "tp"),
        check_vma=False,
    )
```

```python
import functools

import jax
import jax.numpy as jnp
from jax import lax
from jax.experimental import pallas as pl
from jax.experimental.pallas import tpu as pltpu
from jax.sharding import PartitionSpec as P

EPSILON = 1e-06
MESH = pl.DeviceIdType.MESH
PIECES = 2
COLUMN_TILE = 256


def ring_layout(n, n_tp):
    ny = max(n_tp // 2, 1)
    if n % ny or (n // ny) % 2:
        ny = 1
    nz, rest = n // ny, max(ny - 1, 1)

    def position(fs):
        z, y = fs // ny, fs % ny
        k = nz - 1 - z
        odd = k % 2
        back = nz + k * rest + (1 - odd) * (y - 1) + odd * (ny - 1 - y)
        return jnp.where(y == 0, z, back)

    def index(pos):
        q = jnp.maximum(pos - nz, 0)
        k, r = q // rest, q % rest
        odd = k % 2
        back = (nz - 1 - k) * ny + (1 - odd) * (1 + r) + odd * (ny - 1 - r)
        return jnp.where(pos < nz, pos * ny, back)

    return position, index


def kernel(
    n, n_tp, tokens_hbm, norm_gain, gate_hbm, up_hbm, down_hbm, out_gain, out_ref,
    tok, normed, gate, up, down, gate_acc, up_acc, hidden, parts, sib, far, own, sq, sq_all,
    local_sem, ring_send, ring_recv, sib_send, sib_recv, far_send, far_recv, sq_send, sq_recv,
):
    half = n // 2
    nx, cuts = n_tp // 2, down.shape[0] // n
    nb = n * cuts // n_tp
    n_tok, d_model = tok.shape
    rows_in = gate.shape[1]
    n_hid, width = down.shape[1], down.shape[2]
    piece = n_tok // PIECES
    position, index = ring_layout(n, n_tp)
    fs, tp = lax.axis_index("fs"), lax.axis_index("tp")
    x, core = tp // 2, tp % 2
    me = position(fs)
    block_of = {}
    for h in range(half + 1):
        block_of[0, h] = index((me + n - h) % n)
        block_of[1, h] = index((me + h) % n)
    target = (block_of[1, 1], block_of[0, 1])
    sibling = x * 2 + 1 - core

    barrier = pltpu.get_barrier_semaphore()
    for fs_id in target:
        pl.semaphore_signal(barrier, inc=1, device_id={"fs": fs_id}, device_id_type=MESH)
    for d in range(1, n_tp):
        pl.semaphore_signal(
            barrier, inc=1, device_id={"tp": (tp + d) % n_tp}, device_id_type=MESH
        )
    loads = [
        pltpu.make_async_copy(tokens_hbm, tok, local_sem.at[0]),
        pltpu.make_async_copy(gate_hbm, gate.at[fs], local_sem.at[1]),
        pltpu.make_async_copy(up_hbm, up.at[fs], local_sem.at[2]),
    ]
    for j in range(cuts):
        cols = pl.ds(j * width, width)
        loads.append(
            pltpu.make_async_copy(
                down_hbm.at[:, cols], down.at[fs * cuts + j], local_sem.at[3 + j]
            )
        )
    for load in loads:
        load.start()
    pl.semaphore_wait(barrier, 2 + n_tp - 1)

    def view(c, b, h, way):
        if c < 2:
            ref = (gate, up)[c]
            if h == half:
                return ref.at[b, pl.ds(way * (rows_in // 2), rows_in // 2)]
            return ref.at[b]
        if h == half:
            return down.at[b * cuts + c - 2, pl.ds(way * (n_hid // 2), n_hid // 2)]
        return down.at[b * cuts + c - 2]

    def ring_copy(c, way, h, b, first=False):
        dst = view(c, b, h, way)
        src = (gate_hbm, up_hbm)[c] if first and c < 2 else dst
        return pltpu.make_async_remote_copy(
            src_ref=src,
            dst_ref=dst,
            send_sem=ring_send.at[way, h - 1, c],
            recv_sem=ring_recv.at[way, h - 1, c],
            device_id={"fs": target[way]},
            device_id_type=MESH,
        )

    sends = []

    def send(c, way, h):
        copy = ring_copy(c, way, h, block_of[way, h - 1], h == 1)
        copy.start()
        sends.append(copy)

    def arrive(c, way, h):
        ring_copy(c, way, h, block_of[way, h]).wait_recv()

    for c in (0, 1):
        for way in (0, 1):
            send(c, way, 1)

    loads[0].wait()
    tile = min(128, n_tok)

    @pl.loop(0, n_tok // tile)
    def _(i):
        rows = pl.ds(pl.multiple_of(i * tile, tile), tile)
        v = tok[rows, :].astype(jnp.float32)
        r = lax.rsqrt(jnp.mean(v * v, axis=1, keepdims=True) + EPSILON)
        out = (v * r * norm_gain[...]).astype(jnp.bfloat16)
        for j in range(n):
            normed[j, rows, :] = out[:, j * rows_in:(j + 1) * rows_in]

    def accumulate(b, mode):
        n_col = gate.shape[2]
        step = min(COLUMN_TILE, n_col)

        @pl.loop(0, n_col // step)
        def _(i):
            cols = pl.ds(pl.multiple_of(i * step, step), step)
            a = normed[b]
            g = jnp.dot(a, gate[b, :, cols], preferred_element_type=jnp.float32)
            u = jnp.dot(a, up[b, :, cols], preferred_element_type=jnp.float32)
            if mode != "first":
                g = g + gate_acc[:, cols]
                u = u + up_acc[:, cols]
            if mode == "last":
                hidden[:, cols] = (g * (1.0 / (1.0 + jnp.exp(-g))) * u).astype(jnp.bfloat16)
            else:
                gate_acc[:, cols] = g
                up_acc[:, cols] = u

    loads[1].wait()
    loads[2].wait()
    accumulate(fs, "first")
    for load in loads[3:]:
        load.wait()

    for h in range(1, half + 1):
        for c in (0, 1):
            for way in (0, 1):
                arrive(c, way, h)
                if h < half:
                    send(c, way, h + 1)
        if h == half - 1:
            for j in range(cuts):
                for way in (0, 1):
                    send(2 + j, way, 1)
        if h < half:
            accumulate(block_of[0, h], "mid")
            accumulate(block_of[1, h], "mid")
        else:
            accumulate(block_of[0, h], "last")

    def owner(b):
        t = b // nb
        return t // 2, t % 2, b % nb

    def piece_rows(q):
        return pl.ds(pl.multiple_of(q * piece, piece), piece)

    def sib_copy(b, slot, q):
        return pltpu.make_async_remote_copy(
            src_ref=parts.at[b, piece_rows(q)],
            dst_ref=sib.at[slot, piece_rows(q)],
            send_sem=sib_send.at[slot, q],
            recv_sem=sib_recv.at[slot, q],
            device_id={"tp": sibling},
            device_id_type=MESH,
        )

    def far_copy(b, x_to, x_from, k, q):
        return pltpu.make_async_remote_copy(
            src_ref=parts.at[b, piece_rows(q)],
            dst_ref=far.at[x_from, k, piece_rows(q)],
            send_sem=far_send.at[x_to * nb + k, q],
            recv_sem=far_recv.at[x_from, k, q],
            device_id={"tp": x_to * 2 + core},
            device_id_type=MESH,
        )

    def multiply(b):
        x_to, core_to, k = owner(b)

        @pl.loop(0, PIECES)
        def _(q):
            rows = piece_rows(q)
            parts[b, rows, :] = jnp.dot(
                hidden[rows, :], down[b], preferred_element_type=jnp.float32
            ).astype(jnp.bfloat16)

            @pl.when(core_to != core)
            def _():
                sib_copy(b, x_to * nb + k, q).start()

    def reduce(b):
        x_to, core_to, k = owner(b)

        @pl.when((core_to == core) & (x_to != x))
        def _():
            @pl.loop(0, PIECES)
            def _(q):
                rows = piece_rows(q)
                slot = x_to * nb + k
                sib_copy(b, slot, q).wait_recv()
                parts[b, rows, :] = (
                    parts[b, rows, :].astype(jnp.float32) + sib[slot, rows, :].astype(jnp.float32)
                ).astype(jnp.bfloat16)
                far_copy(b, x_to, x, k, q).start()

    ready = [fs * cuts + j for j in range(cuts)]
    for h in range(1, half + 1):
        for j in range(cuts):
            for way in (0, 1):
                arrive(2 + j, way, h)
                if h < half:
                    send(2 + j, way, h + 1)
            for way in (0, 1) if h < half else (0,):
                ready.append(block_of[way, h] * cuts + j)
            for b in ready:
                multiply(b)
            for b in ready:
                reduce(b)
            ready = []

    @pl.loop(0, PIECES)
    def _(q):
        rows = piece_rows(q)
        squares = jnp.zeros((piece, 1), jnp.float32)
        for k in range(nb):
            b, slot = tp * nb + k, x * nb + k
            v = parts[b, rows, :].astype(jnp.float32)
            sib_copy(b, slot, q).wait_recv()
            v = v + sib[slot, rows, :].astype(jnp.float32)
            for d in range(1, nx):
                x_from = (x + d) % nx
                far_copy(b, x, x_from, k, q).wait_recv()
                v = v + far[x_from, k, rows, :].astype(jnp.float32)
            own[k, rows, :] = v
            squares = squares + jnp.sum(v * v, axis=1, keepdims=True)
        sq[q] = jnp.transpose(jnp.broadcast_to(squares, (piece, 128)))[0:8, :]

    def sq_copy(to, slot):
        return pltpu.make_async_remote_copy(
            src_ref=sq,
            dst_ref=sq_all.at[slot],
            send_sem=sq_send.at[to],
            recv_sem=sq_recv.at[slot],
            device_id={"tp": to},
            device_id_type=MESH,
        )

    others = [(tp + d) % n_tp for d in range(1, n_tp)]
    for t in others:
        sq_copy(t, tp).start()
    for t in others:
        sq_copy(t, t).wait_recv()

    @pl.loop(0, PIECES)
    def _(q):
        rows = piece_rows(q)
        total = sq[q]
        for t in others:
            total = total + sq_all[t, q]
        r = lax.rsqrt(total / d_model + EPSILON)
        r = jnp.transpose(jnp.broadcast_to(r[0:1, :], (128, piece)))[:, 0:1]
        for k in range(nb):
            cols = slice(k * width, (k + 1) * width)
            out_ref[rows, cols] = (own[k, rows, :] * r * out_gain[:, cols]).astype(jnp.bfloat16)

    for t in others:
        sq_copy(t, tp).wait_send()
    for copy in sends:
        copy.wait_send()

    @pl.loop(0, PIECES)
    def _(q):
        for slot in range(nx * nb):
            sib_copy(slot, slot, q).wait_send()
        for d in range(1, nx):
            for k in range(nb):
                far_copy(k, (x + d) % nx, x, k, q).wait_send()


def body(n, n_tp, tokens, norm_gain, gate_weight, up_weight, down_weight, out_gain):
    n_tok, d_model = tokens.shape
    rows_in, n_hid = gate_weight.shape
    cuts = max(down_weight.shape[1] // 128, 1)
    width = down_weight.shape[1] // cuts
    half, nx, nb = n // 2, n_tp // 2, n * cuts // n_tp
    piece = n_tok // PIECES
    bf16, f32 = jnp.bfloat16, jnp.float32
    dma = pltpu.SemaphoreType.DMA
    hbm = pl.BlockSpec(memory_space=pl.ANY)
    vmem = pl.BlockSpec(memory_space=pltpu.VMEM)
    return pl.pallas_call(
        functools.partial(kernel, n, n_tp),
        out_shape=jax.ShapeDtypeStruct((n_tok, out_gain.shape[0]), bf16),
        in_specs=[hbm, vmem, hbm, hbm, hbm, vmem],
        out_specs=vmem,
        scratch_shapes=[
            pltpu.VMEM((n_tok, d_model), bf16),
            pltpu.VMEM((n, n_tok, rows_in), bf16),
            pltpu.VMEM((n, rows_in, n_hid), bf16),
            pltpu.VMEM((n, rows_in, n_hid), bf16),
            pltpu.VMEM((n * cuts, n_hid, width), bf16),
            pltpu.VMEM((n_tok, n_hid), f32),
            pltpu.VMEM((n_tok, n_hid), f32),
            pltpu.VMEM((n_tok, n_hid), bf16),
            pltpu.VMEM((n * cuts, n_tok, width), bf16),
            pltpu.VMEM((nx * nb, n_tok, width), bf16),
            pltpu.VMEM((nx, nb, n_tok, width), bf16),
            pltpu.VMEM((nb, n_tok, width), f32),
            pltpu.VMEM((PIECES, 8, piece), f32),
            pltpu.VMEM((n_tp, PIECES, 8, piece), f32),
            dma((3 + cuts,)),
            dma((2, half, 2 + cuts)),
            dma((2, half, 2 + cuts)),
            dma((nx * nb, PIECES)),
            dma((nx * nb, PIECES)),
            dma((nx * nb, PIECES)),
            dma((nx, nb, PIECES)),
            dma((n_tp,)),
            dma((n_tp,)),
        ],
        compiler_params=pltpu.CompilerParams(
            collective_id=0, has_side_effects=True, vmem_limit_bytes=62 * 1024 * 1024
        ),
        name="ffn_ring",
    )(tokens, norm_gain[None, :], gate_weight, up_weight, down_weight, out_gain[None, :])


def solution(mesh):
    return jax.shard_map(
        functools.partial(body, mesh.shape["fs"], mesh.shape["tp"]),
        mesh=mesh,
        in_specs=(P("fs", None), P(), P("fs", "tp"), P("fs", "tp"), P("tp", "fs"), P("tp")),
        out_specs=P("fs", "tp"),
        check_vma=False,
    )
```
